32 devices in a mesh: sp: 8 (over z, y), tp: 4 (over x, core).
Axes of the slice: x: 2, y: 2, z: 4, core: 2. Of those that a mesh axis runs over, the one named last changes fastest.
Arguments:
- queries: bfloat16 [4096, 1024], P('sp', 'tp'), may hold values from -6 to 6
- key_heads: bfloat16 [4096, 512], P('sp', 'tp'), may hold values from -6 to 6
- value_heads: bfloat16 [4096, 512], P('sp', 'tp'), may hold values from -70 to 70
- documents: int32 [4096], P('sp'), may hold values from 0 to 2, never falling along the last dimension, each value on 1 to 2560 neighbouring positions
- query_gain: float32 [128], replicated, may hold values from 0.1 to 8
- key_gain: float32 [128], replicated, may hold values from 0.1 to 8
- out_gain: float32 [1024], replicated, may hold values from 0.1 to 1.9
- out_proj: bfloat16 [1024, 2048], replicated, may hold values from -0.1875 to 0.1875
- residual: bfloat16 [4096, 2048], P(('sp', 'tp')), may hold values from -6 to 6
- mid_gain: float32 [2048], replicated, may hold values from 0.1 to 1.9
- mid_bias: float32 [2048], replicated, may hold values from -1.5 to 1.5
- routes: int32 [4096, 2], P(('sp', 'tp')), may hold values from 0 to 31, all different within a row; in each aligned block of 128 rows (0 to 127, 128 to 255, ...) at most 16 rows name the same one
- route_weights: float32 [4096, 2], P(('sp', 'tp')), may hold values from 0.2 to 2
- expert_gate: bfloat16 [32, 2048, 512], P(('sp', 'tp')), may hold values from -0.125 to 0.125
- expert_up: bfloat16 [32, 2048, 512], P(('sp', 'tp')), may hold values from -0.125 to 0.125
- expert_down: bfloat16 [32, 512, 2048], P(('sp', 'tp')), may hold values from -0.25 to 0.25
- final_gain: float32 [2048], replicated, may hold values from 0.1 to 1.9
- final_bias: float32 [2048], replicated, may hold values from -1.5 to 1.5
Outputs:
- layer_out: bfloat16 [4096, 2048], P(('sp', 'tp'))
The draws below stay inside these ranges and needn't reach their ends.
Inputs may be any that keep to these rules, and one draw needn't show every extreme that they name: `documents`: never falls along the sequence; each document holds 1 to 2560 positions and one holds exactly 2560. `routes`: each row names 2 different experts; among the rows of one device (aligned blocks of 128 rows) no expert is named more than 16 times, and exactly 16 times in some block.
All inputs are finite; a program needn't handle non-finite values.
Results may differ from the reference program's by a relative error of at most 0.014.
The reference program's roundings to bfloat16 on the way count: a program that leaves them out, or rounds other values in their place, can miss the bound.
Values may be sent and summed in bfloat16 or wider, within the bound.
A program may use at most 128 MiB of HBM per device.

```python
import math
import jax
import jax.numpy as jnp
import numpy as np
from jax import lax

D = 2048
HEAD = 128
QH = 8
KVH = 4
GRID = 64
DE = 512
TOP_K = 2
TOKENS = 4096
ROWS = 128
EXPERTS = 32
CAP = 16
DOCS = 3
DOC_MOST = 2560
N_SP = 8
N_TP = 4


def drawn_keys(key):
    sub_key = jax.random.fold_in(key, 202)
    drawn = jnp.clip(jax.random.normal(sub_key, (TOKENS, KVH * HEAD), jnp.float32), -6.0, 6.0)
    return drawn


def draw_key_heads(key, part):
    return drawn_keys(key).astype(jnp.bfloat16)


def draw_queries(key, part):
    sub_key = jax.random.fold_in(key, 301)
    drawn = jnp.clip(jax.random.normal(sub_key, (TOKENS, QH * HEAD), jnp.float32), -6.0, 6.0)
    return drawn.astype(jnp.bfloat16)


def draw_value_heads(key, part):
    sub_key = jax.random.fold_in(key, 501)
    head_index = jnp.arange(KVH, dtype=jnp.float32)
    head_scale = jnp.repeat(4.0 ** (head_index / (KVH - 1)), HEAD)
    drawn = jnp.clip(jax.random.normal(sub_key, (TOKENS, KVH * HEAD), jnp.float32), -4.0, 4.0)
    return (drawn * head_scale[None, :]).astype(jnp.bfloat16)


def gain_values(key):
    return jnp.clip(1.0 + 0.18 * jax.random.normal(key, (HEAD,), jnp.float32), 0.1, 1.9)


def draw_query_gain(key, part):
    return gain_values(jax.random.fold_in(key, 401))


def draw_key_gain(key, part):
    return gain_values(jax.random.fold_in(key, 402))


def levels(stream_key, shape, shards, smallest, largest):
    loudness, own = 1.0, jax.random.fold_in(stream_key, 6)
    for position, shards_of in shards:
        heights = jnp.exp(jax.random.uniform(jax.random.fold_in(own, position), (shards_of,), jnp.float32, smallest / len(shards), largest / len(shards)))
        loudness = loudness * jnp.repeat(heights, shape[position] // shards_of).reshape([-1 if axis == position else 1 for axis in range(len(shape))])
    return loudness


def profile(amount, total, limit, skew):
    portions = [(1 << 20) // math.isqrt(rank ** skew) + 1 for rank in range(2, amount + 1)]
    surplus, holding = total - limit - (amount - 1), [1] * (amount - 1)
    while surplus > 0:
        movable = [i for i in range(amount - 1) if holding[i] < limit]
        whole, left = sum([portions[i] for i in movable]), surplus
        for i in movable:
            extra = min(limit - holding[i], max(1, left * portions[i] // whole), surplus)
            holding[i] = holding[i] + extra
            surplus = surplus - extra
    return np.array([limit] + holding)


def uneven_parts(rng, amount, total, limit, skew):
    if amount == 2:
        one = jax.random.randint(rng, (), max(1, total - limit), min(limit, total - 1) + 1)
        return jnp.stack([one, total - one])
    tallies = jnp.asarray(profile(amount, total, limit, skew), jnp.int32)
    twos = (amount - 1) // 2
    donor, taker = tallies[1:1 + 2 * twos:2], tallies[2:2 + 2 * twos:2]
    room = jnp.minimum(donor - 1, limit - taker)
    passed = jax.random.randint(jax.random.fold_in(rng, 1), (twos,), 0, 1 << 20) % (room + 1)
    tallies = tallies.at[1:1 + 2 * twos:2].set(donor - passed).at[2:2 + 2 * twos:2].set(taker + passed)
    return tallies[jax.random.permutation(jax.random.fold_in(rng, 2), amount)]


def assign_block(key, own, number, rows, number_of, top, limit, slope):
    order = jax.random.permutation(key, number_of)
    crowded, common = portions_of(number_of, rows * top, limit, slope, True), portions_of(number_of, rows * top, limit, slope, False)
    places = jnp.arange(number_of)

    def named(sizes, offset_by):
        used = int((sizes > 0).sum())
        fixed = max(1, used // 4)
        passed = fixed + (places - fixed + offset_by * (used - fixed)) % max(1, number_of - fixed)
        return jnp.zeros((number_of,), jnp.int32).at[order[jnp.where(places < fixed, places, passed)]].set(jnp.asarray(sizes, jnp.int32))

    sizes = jnp.where(number % 4 == 0, named(crowded, number // 4), named(common, number - number // 4 - 1))
    mixed = jax.random.permutation(jax.random.fold_in(own, 3), number_of)
    giver, receiver = mixed[0:number_of // 2 * 2:2], mixed[1:number_of // 2 * 2:2]
    slack = jnp.minimum(sizes[giver] - 1, limit - sizes[receiver]) // 2
    slack = jnp.where((giver == order[0]) | (receiver == order[0]) | (sizes[receiver] == 0), 0, jnp.maximum(slack, 0))
    passed = jax.random.randint(jax.random.fold_in(own, 4), (number_of // 2,), 0, 1 << 20) % (slack + 1)
    sizes = sizes.at[giver].add(-passed).at[receiver].add(passed)
    items = jnp.searchsorted(jnp.cumsum(sizes), jnp.arange(rows * top), side="right").astype(jnp.int32)
    table = items.reshape(top, rows).T
    table = table[jax.random.permutation(jax.random.fold_in(own, 1), rows)]
    offset_by = jax.random.randint(jax.random.fold_in(own, 2), (rows, 1), 0, top)
    return jnp.take_along_axis(table, (jnp.arange(top)[None, :] + offset_by) % top, axis=1)


def portions_of(amount, total, most, lean, full):
    loads = [(1 << 20) // math.isqrt(standing ** lean) + 1 for standing in range(1, amount + 1)]
    largest = most if full else min(most, max(-(-total // amount), total * loads[0] // sum(loads)))
    least = 1 if total - largest >= amount - 1 else 0
    given, spare = [largest] + [least] * (amount - 1), total - largest - least * (amount - 1)
    while spare > 0:
        candidates = [i for i in range(1, amount) if given[i] < largest] or [i for i in range(1, amount) if given[i] < most]
        mass, left = sum([loads[i] for i in candidates]), spare
        for i in candidates:
            extra = min(most - given[i], max(1, left * loads[i] // mass), spare)
            given[i] = given[i] + extra
            spare = spare - extra
    return np.array(given)


def gaussian(stream_key, extent, deviation, limit, shards=(), kind=jnp.bfloat16):
    array = deviation * jax.random.normal(stream_key, extent, jnp.float32)
    if shards:
        array = array * levels(stream_key, extent, shards, -0.22, 0.18)
    return jnp.clip(array, -limit, limit).astype(kind)


def setup_inputs(seed: int = 0) -> dict:
    streams_of = jax.random.split(jax.random.key(seed), 19)
    queries = draw_queries(jax.random.fold_in(streams_of[18], 71), 0)
    key_heads = draw_key_heads(jax.random.fold_in(streams_of[18], 71), 0)
    value_heads = draw_value_heads(jax.random.fold_in(streams_of[18], 71), 0)
    documents = jnp.searchsorted(jnp.cumsum(uneven_parts(streams_of[3], DOCS, TOKENS, DOC_MOST, 1)), jnp.arange(TOKENS), side="right").astype(jnp.int32)
    query_gain = draw_query_gain(jax.random.fold_in(streams_of[18], 71), 0)
    key_gain = draw_key_gain(jax.random.fold_in(streams_of[18], 71), 0)
    out_gain = jnp.clip(1.0 + 0.18 * jax.random.normal(streams_of[6], (QH * HEAD,), jnp.float32), 0.1, 1.9)
    out_proj = gaussian(streams_of[7], (QH * HEAD, D), (QH * HEAD) ** -0.5, 0.1875)
    residual = gaussian(streams_of[8], (TOKENS, D), 1.0, 6.0, ((0, 32),))
    mid_gain = jnp.clip(1.0 + 0.18 * jax.random.normal(streams_of[9], (D,), jnp.float32), 0.1, 1.9)
    mid_bias = gaussian(streams_of[10], (D,), 0.3, 1.5, (), jnp.float32)
    routes_keys = jax.random.split(jax.random.fold_in(streams_of[11], 1), TOKENS // ROWS)
    routes_turns = jax.random.permutation(jax.random.fold_in(streams_of[11], 3), TOKENS // ROWS)
    routes = jax.vmap(lambda own, number: assign_block(jax.random.fold_in(streams_of[11], 2), own, number, ROWS, EXPERTS, TOP_K, CAP, 2))(routes_keys, routes_turns).reshape((TOKENS, TOP_K))
    route_weights = jnp.clip(jnp.exp(math.log(2.0) - 2.3025851 * jax.random.uniform(streams_of[12], (TOKENS, TOP_K), jnp.float32) ** levels(streams_of[12], (TOKENS, TOP_K), ((0, 32),), -0.2, 0.2)), 0.2, 2.0)
    expert_gate = gaussian(streams_of[13], (EXPERTS, D, DE), D ** -0.5, 0.125, ((0, 32),))
    expert_up = gaussian(streams_of[14], (EXPERTS, D, DE), D ** -0.5, 0.125, ((0, 32),))
    expert_down = gaussian(streams_of[15], (EXPERTS, DE, D), DE ** -0.5, 0.25, ((0, 32),))
    final_gain = jnp.clip(1.0 + 0.18 * jax.random.normal(streams_of[16], (D,), jnp.float32), 0.1, 1.9)
    final_bias = gaussian(streams_of[17], (D,), 0.3, 1.5, (), jnp.float32)
    return dict(queries=queries, key_heads=key_heads, value_heads=value_heads, documents=documents, query_gain=query_gain, key_gain=key_gain, out_gain=out_gain, out_proj=out_proj, residual=residual, mid_gain=mid_gain, mid_bias=mid_bias, routes=routes, route_weights=route_weights, expert_gate=expert_gate, expert_up=expert_up, expert_down=expert_down, final_gain=final_gain, final_bias=final_bias)


eps_norm = 1e-06
alpha_mix = 8.0 ** 0.25
theta_base = 10000.0

def rotary_tables(row_total, offset):
    positions = offset + jnp.arange(row_total, dtype=jnp.int32)
    grid_row = (positions // GRID).astype(jnp.float32)
    grid_col = (positions % GRID).astype(jnp.float32)
    pair_count = HEAD // 4
    inv_freq = theta_base ** (-jnp.arange(pair_count, dtype=jnp.float32) / pair_count)
    angles = jnp.concatenate([grid_row[:, None] * inv_freq[None, :], grid_col[:, None] * inv_freq[None, :]], axis=1)
    return (jnp.cos(angles), jnp.sin(angles))

def normed_rotated(heads_in, gain_vec, cosine_table, sine_table):
    values = heads_in.astype(jnp.float32)
    inv_rms = lax.rsqrt(lax.optimization_barrier(jnp.mean(values * values, axis=-1, keepdims=True)) + eps_norm)
    values = values * inv_rms * gain_vec
    half_dim = HEAD // 2
    first_half = values[..., :half_dim]
    second_half = values[..., half_dim:]
    cosine_part = cosine_table[:, None, :]
    sine_part = sine_table[:, None, :]
    turned = jnp.concatenate([first_half * cosine_part - second_half * sine_part, second_half * cosine_part + first_half * sine_part], axis=-1)
    return turned.astype(jnp.bfloat16)

def layer_norm(stream, gain_vec, bias_vec):
    center = lax.optimization_barrier(jnp.mean(stream, axis=-1, keepdims=True))
    spread = lax.optimization_barrier(jnp.mean(jnp.square(stream - center), axis=-1, keepdims=True))
    return (stream - center) * lax.rsqrt(spread + eps_norm) * gain_vec + bias_vec

def reference(queries, key_heads, value_heads, documents, query_gain, key_gain, out_gain, out_proj, residual, mid_gain, mid_bias, routes, route_weights, expert_gate, expert_up, expert_down, final_gain, final_bias):
    cosine_table, sine_table = rotary_tables(TOKENS, 0)
    grouped = QH // KVH
    query_rot = normed_rotated(queries.reshape(TOKENS, QH, HEAD), query_gain, cosine_table, sine_table).reshape(TOKENS, KVH, grouped, HEAD)
    key_rot = normed_rotated(key_heads.reshape(TOKENS, KVH, HEAD), key_gain, cosine_table, sine_table).astype(jnp.float32)
    value_all = value_heads.reshape(TOKENS, KVH, HEAD).astype(jnp.float32)
    block_rows = math.gcd(TOKENS, 512)

    def query_block(number):
        first_row = number * block_rows
        query_part = lax.dynamic_slice_in_dim(query_rot, first_row, block_rows, 0).astype(jnp.float32)
        doc_part = lax.dynamic_slice_in_dim(documents, first_row, block_rows, 0)
        scores = jnp.einsum('qkgd,tkd->kgqt', query_part, key_rot) * HEAD ** (-0.5)
        allowed = (doc_part[:, None] == documents[None, :])[None, None]
        scores = jnp.where(allowed, scores, -1e+30)
        row_max = lax.optimization_barrier(jnp.max(scores, axis=-1, keepdims=True))
        weights = jnp.where(allowed, jnp.exp(scores - row_max), 0.0)
        totals = lax.optimization_barrier(jnp.sum(weights, axis=-1))
        rounded = lax.optimization_barrier(weights.astype(jnp.bfloat16)).astype(jnp.float32)
        summed = jnp.einsum('kgqt,tkd->kgqd', rounded, value_all) / totals[..., None]
        return jnp.transpose(summed, (2, 0, 1, 3)).reshape(block_rows, QH * HEAD).astype(jnp.bfloat16)
    attention = lax.map(query_block, jnp.arange(TOKENS // block_rows, dtype=jnp.int32))
    attention = attention.reshape(TOKENS, QH * HEAD)
    attn_float = attention.astype(jnp.float32)
    mean_square = lax.optimization_barrier(jnp.mean(attn_float * attn_float, axis=1, keepdims=True))
    scaled = (attn_float * out_gain).astype(jnp.bfloat16)
    projected = jnp.dot(scaled, out_proj, preferred_element_type=jnp.float32) * lax.rsqrt(mean_square + eps_norm)
    middle = layer_norm(alpha_mix * residual.astype(jnp.float32) + projected, mid_gain, mid_bias).astype(jnp.bfloat16)
    flat_routes = routes.reshape(-1).astype(jnp.int32)
    pair_total = flat_routes.shape[0]
    receive = N_SP * N_TP * CAP
    sorted_order = jnp.argsort(flat_routes, stable=True).astype(jnp.int32)
    counts = lax.optimization_barrier(jnp.sum((flat_routes[:, None] == jnp.arange(EXPERTS, dtype=jnp.int32)[None, :]).astype(jnp.int32), axis=0))
    starts = jnp.cumsum(counts) - counts
    inverse = jnp.zeros((pair_total,), jnp.int32).at[sorted_order].set(jnp.arange(pair_total, dtype=jnp.int32))
    token_of = sorted_order // TOP_K

    def expert_pass(expert):
        slot_index = starts[expert] + jnp.arange(receive, dtype=jnp.int32)
        live_rows = slot_index < starts[expert] + counts[expert]
        source_rows = middle[token_of[jnp.minimum(slot_index, pair_total - 1)]]
        picked = jnp.where(live_rows[:, None], source_rows, jnp.zeros((), jnp.bfloat16))
        gate_part = jnp.dot(picked, expert_gate[expert], preferred_element_type=jnp.float32)
        up_part = jnp.dot(picked, expert_up[expert], preferred_element_type=jnp.float32)
        hidden = (jax.nn.silu(gate_part) * up_part).astype(jnp.bfloat16)
        return jnp.dot(hidden, expert_down[expert], preferred_element_type=jnp.float32).astype(jnp.bfloat16)
    served = lax.map(expert_pass, jnp.arange(EXPERTS, dtype=jnp.int32)).reshape(EXPERTS * receive, D)
    slot_rows = flat_routes * receive + (inverse - starts[flat_routes])
    gathered = served[slot_rows].astype(jnp.float32).reshape(TOKENS, TOP_K, D)
    routed = lax.optimization_barrier(jnp.sum(gathered * route_weights[:, :, None], axis=1))
    return layer_norm(alpha_mix * middle.astype(jnp.float32) + routed, final_gain, final_bias).astype(jnp.bfloat16)
```

```python
import functools

import jax
import jax.numpy as jnp
from jax import lax
from jax.experimental import pallas as pl
from jax.experimental.pallas import tpu as pltpu
from jax.sharding import PartitionSpec as P

HEAD = 128
GRID = 64


eps_norm = 1e-06
alpha_mix = 8.0**0.25
theta_base = 10000.0
score_factor = HEAD ** (-0.5) * 1.4426950408889634
VMEM = pl.BlockSpec(memory_space=pltpu.VMEM)
ANY = pl.BlockSpec(memory_space=pl.ANY)
SMEM = pl.BlockSpec(memory_space=pltpu.SMEM)


def rotary_tables(row_total, offset):
    positions = offset + jnp.arange(row_total, dtype=jnp.int32)
    grid_row = (positions // GRID).astype(jnp.float32)
    grid_col = (positions % GRID).astype(jnp.float32)
    pair_count = HEAD // 4
    inv_freq = theta_base ** (-jnp.arange(pair_count, dtype=jnp.float32) / pair_count)
    angles = jnp.concatenate(
        [grid_row[:, None] * inv_freq[None, :], grid_col[:, None] * inv_freq[None, :]], axis=1
    )
    return (jnp.cos(angles), jnp.sin(angles))


def normed_rotated(heads_in, gain_vec, cosine_table, sine_table):
    values = heads_in.astype(jnp.float32)
    inv_rms = lax.rsqrt(jnp.mean(values * values, axis=-1, keepdims=True) + eps_norm)
    values = values * inv_rms * gain_vec
    half_dim = HEAD // 2
    first_half = values[..., :half_dim]
    second_half = values[..., half_dim:]
    cosine_part = cosine_table[:, None, :]
    sine_part = sine_table[:, None, :]
    turned = jnp.concatenate(
        [
            first_half * cosine_part - second_half * sine_part,
            second_half * cosine_part + first_half * sine_part,
        ],
        axis=-1,
    )
    return turned.astype(jnp.bfloat16)


def layer_norm(stream, gain_vec, bias_vec):
    center = jnp.mean(stream, axis=-1, keepdims=True)
    spread = jnp.mean(jnp.square(stream - center), axis=-1, keepdims=True)
    return (stream - center) * lax.rsqrt(spread + eps_norm) * gain_vec + bias_vec


def barrier_with(peers):
    barrier = pltpu.get_barrier_semaphore()
    for peer in peers:
        pl.semaphore_signal(barrier, inc=1, device_id=peer, device_id_type=pl.DeviceIdType.MESH)
    pl.semaphore_wait(barrier, len(peers))


def gather_kernel(
    size, pair, kv_ref, doc_ref, kv_all, doc_all, kv_send, kv_recv, doc_send, doc_recv, own_sem
):
    me = lax.axis_index("sp")
    inner = lax.rem(me, pair)
    outer = me // pair
    outer_size = size // pair
    own = [
        pltpu.make_async_copy(kv_ref, kv_all.at[me], own_sem.at[0]),
        pltpu.make_async_copy(doc_ref, doc_all.at[me], own_sem.at[1]),
    ]
    for copy in own:
        copy.start()
    far = [
        lax.rem(outer + step, outer_size) * pair + inner for step in range(1, outer_size)
    ]
    mate = outer * pair + lax.rem(inner + 1, pair)
    peers = [{"sp": index} for index in far]
    if pair == 2:
        peers.append({"sp": mate})
    barrier_with(peers)

    def send(from_kv, from_doc, place, slot, target):
        copies = (
            pltpu.make_async_remote_copy(
                src_ref=from_kv,
                dst_ref=kv_all.at[place],
                send_sem=kv_send.at[slot],
                recv_sem=kv_recv.at[slot],
                device_id={"sp": target},
                device_id_type=pl.DeviceIdType.MESH,
            ),
            pltpu.make_async_remote_copy(
                src_ref=from_doc,
                dst_ref=doc_all.at[place],
                send_sem=doc_send.at[slot],
                recv_sem=doc_recv.at[slot],
                device_id={"sp": target},
                device_id_type=pl.DeviceIdType.MESH,
            ),
        )
        for copy in copies:
            copy.start()
        return copies

    far_copies = []
    for step, target in enumerate(far):
        far_copies.append(send(kv_ref, doc_ref, me, step, target))
    mate_copies = []
    if pair == 2:
        mate_copies.append(send(kv_ref, doc_ref, me, outer_size - 1, mate))
    for step in range(1, outer_size):
        for copy in far_copies[step - 1]:
            copy.wait_recv()
        if pair == 2:
            place = lax.rem(outer - step + outer_size, outer_size) * pair + inner
            mate_copies.append(
                send(kv_all.at[place], doc_all.at[place], place, outer_size - 1 + step, mate)
            )
    for copies in mate_copies:
        for copy in copies:
            copy.wait_recv()
    for copies in far_copies + mate_copies:
        for copy in copies:
            copy.wait_send()
    for copy in own:
        copy.wait()


def gather_keys(kv, docs, size):
    pair = 2 if size % 2 == 0 else 1
    slots = max(size - 1, 1)
    return pl.pallas_call(
        functools.partial(gather_kernel, size, pair),
        out_shape=(
            jax.ShapeDtypeStruct((size,) + kv.shape, kv.dtype),
            jax.ShapeDtypeStruct((size,) + docs.shape, docs.dtype),
        ),
        in_specs=[ANY, ANY],
        out_specs=(ANY, ANY),
        scratch_shapes=[pltpu.SemaphoreType.DMA((slots,)) for unused in range(4)]
        + [pltpu.SemaphoreType.DMA((2,))],
        compiler_params=pltpu.CompilerParams(collective_id=0, has_side_effects=True),
    )(kv, docs)


def attention_kernel(grouped, q_ref, qdoc_ref, kv_ref, doc_ref, range_ref, o_ref, m_ref, l_ref, acc_ref):
    rows = q_ref.shape[1]
    block = kv_ref.shape[2]
    pieces = doc_ref.shape[1]
    chunk = 256
    m_ref[...] = jnp.full(m_ref.shape, -1e30, jnp.float32)
    l_ref[...] = jnp.zeros(l_ref.shape, jnp.float32)
    acc_ref[...] = jnp.zeros(acc_ref.shape, jnp.float32)

    def advance(number, unused):
        keys = kv_ref[number, 0]
        values = kv_ref[number, 1]
        doc_rows = doc_ref[number]
        key_docs = jnp.concatenate([doc_rows[i : i + 1] for i in range(pieces)], axis=1)
        for head in range(grouped):
            for first in range(0, rows, chunk):
                part = pl.ds(first, chunk)
                scores = lax.dot_general(
                    q_ref[head, part],
                    keys,
                    (((1,), (1,)), ((), ())),
                    preferred_element_type=jnp.float32,
                )
                allowed = qdoc_ref[part, 0:1] == key_docs
                scores = jnp.where(allowed, scores * score_factor, -1e30)
                old_max = m_ref[head, part]
                new_max = jnp.maximum(old_max, jnp.max(scores, axis=1, keepdims=True))
                base = jnp.maximum(new_max[:, 0:1], -1e29)
                weights = jnp.exp2(scores - base)
                rescale = jnp.exp2(old_max - new_max)
                l_ref[head, part] = l_ref[head, part] * rescale + jnp.sum(
                    weights, axis=1, keepdims=True
                )
                acc_ref[head, part] = acc_ref[head, part] * rescale + jnp.dot(
                    weights.astype(jnp.bfloat16), values, preferred_element_type=jnp.float32
                )
                m_ref[head, part] = new_max
        return unused

    lax.fori_loop(range_ref[0], range_ref[1], advance, 0)
    for head in range(grouped):
        o_ref[:, head * HEAD : (head + 1) * HEAD] = (acc_ref[head] / l_ref[head]).astype(
            o_ref.dtype
        )


def attend(query_rot, query_docs, kv_all, doc_all, block_range):
    grouped, rows, width = query_rot.shape
    return pl.pallas_call(
        functools.partial(attention_kernel, grouped),
        out_shape=jax.ShapeDtypeStruct((rows, grouped * width), jnp.bfloat16),
        in_specs=[VMEM, VMEM, VMEM, VMEM, SMEM],
        out_specs=VMEM,
        scratch_shapes=[pltpu.VMEM((grouped, rows, width), jnp.float32) for unused in range(3)],
        compiler_params=pltpu.CompilerParams(vmem_limit_bytes=48 * 1024 * 1024),
    )(query_rot, query_docs, kv_all, doc_all, block_range)


def head_exchange_kernel(size, x_ref, o_ref, send_sem, recv_sem, own_sem):
    me = lax.axis_index("tp")
    rows, width = o_ref.shape[0], x_ref.shape[1]
    mine = o_ref.at[:, pl.ds(pl.multiple_of(me * width, width), width)]
    own = pltpu.make_async_copy(
        x_ref.at[pl.ds(pl.multiple_of(me * rows, rows), rows)], mine, own_sem
    )
    own.start()
    targets = [lax.rem(me + step, size) for step in range(1, size)]
    barrier_with([{"tp": target} for target in targets])
    copies = []
    for step, target in enumerate(targets):
        copy = pltpu.make_async_remote_copy(
            src_ref=x_ref.at[pl.ds(pl.multiple_of(target * rows, rows), rows)],
            dst_ref=mine,
            send_sem=send_sem.at[step],
            recv_sem=recv_sem.at[step],
            device_id={"tp": target},
            device_id_type=pl.DeviceIdType.MESH,
        )
        copy.start()
        copies.append(copy)
    for copy in copies:
        copy.wait()
    own.wait()


def exchange_heads(attention, size):
    rows, width = attention.shape
    return pl.pallas_call(
        functools.partial(head_exchange_kernel, size),
        out_shape=jax.ShapeDtypeStruct((rows // size, width * size), attention.dtype),
        in_specs=[VMEM],
        out_specs=VMEM,
        scratch_shapes=[
            pltpu.SemaphoreType.DMA((size,)),
            pltpu.SemaphoreType.DMA((size,)),
            pltpu.SemaphoreType.DMA,
        ],
        compiler_params=pltpu.CompilerParams(collective_id=1, has_side_effects=True),
    )(attention)


def all_exchange_kernel(sp_size, tp_size, x_ref, o_ref, send_sem, recv_sem, own_sem):
    me = lax.axis_index("sp") * tp_size + lax.axis_index("tp")
    size = sp_size * tp_size
    own = pltpu.make_async_copy(x_ref.at[me], o_ref.at[me], own_sem)
    own.start()
    barrier = pltpu.get_barrier_semaphore()

    def greet(step, unused):
        target = lax.rem(me + step, size)
        pl.semaphore_signal(
            barrier,
            inc=1,
            device_id={"sp": target // tp_size, "tp": lax.rem(target, tp_size)},
            device_id_type=pl.DeviceIdType.MESH,
        )
        return unused

    lax.fori_loop(1, size, greet, 0)
    pl.semaphore_wait(barrier, size - 1)

    def copy_of(step):
        target = lax.rem(me + step, size)
        return pltpu.make_async_remote_copy(
            src_ref=x_ref.at[target],
            dst_ref=o_ref.at[me],
            send_sem=send_sem.at[step],
            recv_sem=recv_sem.at[step],
            device_id={"sp": target // tp_size, "tp": lax.rem(target, tp_size)},
            device_id_type=pl.DeviceIdType.MESH,
        )

    def begin(step, unused):
        copy_of(step).start()
        return unused

    def finish(step, unused):
        copy_of(step).wait()
        return unused

    lax.fori_loop(1, size, begin, 0)
    lax.fori_loop(1, size, finish, 0)
    own.wait()


def exchange_all(blocks, sp_size, tp_size, collective_id):
    size = blocks.shape[0]
    return pl.pallas_call(
        functools.partial(all_exchange_kernel, sp_size, tp_size),
        out_shape=jax.ShapeDtypeStruct(blocks.shape, blocks.dtype),
        in_specs=[ANY],
        out_specs=ANY,
        scratch_shapes=[
            pltpu.SemaphoreType.DMA((size,)),
            pltpu.SemaphoreType.DMA((size,)),
            pltpu.SemaphoreType.DMA,
        ],
        compiler_params=pltpu.CompilerParams(collective_id=collective_id, has_side_effects=True),
    )(blocks)


def middle_kernel(
    x_ref, gain_ref, proj_ref, res_ref, mid_gain_ref, mid_bias_ref, target_ref, mid_ref, out_ref
):
    whole = x_ref[...].astype(jnp.float32)
    mean_square = jnp.mean(whole * whole, axis=1, keepdims=True)
    scaled = (whole * gain_ref[...]).astype(jnp.bfloat16)
    projected = jnp.dot(scaled, proj_ref[...], preferred_element_type=jnp.float32)
    projected = projected * lax.rsqrt(mean_square + eps_norm)
    stream = alpha_mix * res_ref[...].astype(jnp.float32) + projected
    middle = layer_norm(stream, mid_gain_ref[...], mid_bias_ref[...]).astype(jnp.bfloat16)
    mid_ref[...] = middle
    slots, rows = out_ref.shape[0], middle.shape[0]
    slot = lax.broadcasted_iota(jnp.int32, (slots, rows), 0)
    chosen = slot == target_ref[0:1, :]
    for route in range(1, target_ref.shape[0]):
        chosen = chosen | (slot == target_ref[route : route + 1, :])
    select = jnp.where(chosen, 1.0, 0.0).astype(jnp.bfloat16)
    out_ref[...] = jnp.dot(select, middle, preferred_element_type=jnp.float32).astype(
        jnp.bfloat16
    )


def final_kernel(back_ref, target_ref, weight_ref, mid_ref, gain_ref, bias_ref, o_ref):
    rows, slots = mid_ref.shape[0], back_ref.shape[0]
    slot = lax.broadcasted_iota(jnp.int32, (rows, slots), 1)
    routed = None
    for route in range(target_ref.shape[1]):
        select = jnp.where(slot == target_ref[:, route : route + 1], 1.0, 0.0)
        picked = jnp.dot(
            select.astype(jnp.bfloat16), back_ref[...], preferred_element_type=jnp.float32
        )
        term = picked * weight_ref[:, route : route + 1]
        routed = term if routed is None else routed + term
    stream = alpha_mix * mid_ref[...].astype(jnp.float32) + routed
    o_ref[...] = layer_norm(stream, gain_ref[...], bias_ref[...]).astype(o_ref.dtype)


def per_device(
    queries,
    key_heads,
    value_heads,
    documents,
    query_gain,
    key_gain,
    out_gain,
    out_proj,
    residual,
    mid_gain,
    mid_bias,
    routes,
    route_weights,
    expert_gate,
    expert_up,
    expert_down,
    final_gain,
    final_bias,
):
    tok_rows = queries.shape[0]
    query_local = queries.shape[1] // HEAD
    key_local = key_heads.shape[1] // HEAD
    grouped = query_local // key_local
    sp_size = lax.axis_size("sp")
    tp_size = lax.axis_size("tp")
    offset = lax.axis_index("sp") * tok_rows
    cosine_table, sine_table = rotary_tables(tok_rows, offset)
    query_rot = normed_rotated(
        queries.reshape(tok_rows, query_local, HEAD), query_gain, cosine_table, sine_table
    )
    query_rot = jnp.transpose(query_rot, (1, 0, 2))
    key_rot = normed_rotated(
        key_heads.reshape(tok_rows, key_local, HEAD), key_gain, cosine_table, sine_table
    )
    values = value_heads.reshape(tok_rows, key_local, HEAD)
    query_docs = jnp.broadcast_to(documents[:, None], (tok_rows, HEAD))
    kv = jnp.transpose(jnp.stack([key_rot, values]), (2, 0, 1, 3))
    kv_all, doc_all = gather_keys(
        kv.reshape(key_local * 2, tok_rows, HEAD), documents.reshape(tok_rows // HEAD, HEAD), sp_size
    )
    low = jnp.sum((doc_all[:, -1, -1] < documents[0]).astype(jnp.int32))
    high = jnp.sum((doc_all[:, 0, 0] <= documents[tok_rows - 1]).astype(jnp.int32))
    block_range = jnp.stack([low, high])
    heads = []
    for head in range(key_local):
        heads.append(
            attend(
                query_rot[head * grouped : (head + 1) * grouped],
                query_docs,
                kv_all if key_local == 1 else kv_all[:, 2 * head : 2 * head + 2],
                doc_all,
                block_range,
            )
        )
    attention = heads[0] if key_local == 1 else jnp.concatenate(heads, axis=1)
    whole_rows = exchange_heads(attention, tp_size)
    out_rows, model_width = residual.shape
    top_count = routes.shape[1]
    local_experts = expert_gate.shape[0]
    device_total = sp_size * tp_size
    expert_total = local_experts * device_total
    capacity = 2 * out_rows * top_count // expert_total
    flat_routes = routes.T.reshape(-1)
    flat_total = flat_routes.shape[0]
    one_hot = flat_routes[:, None] == jnp.arange(expert_total, dtype=jnp.int32)[None, :]
    earlier = jnp.arange(flat_total)[:, None] > jnp.arange(flat_total)[None, :]
    before = jnp.dot(
        earlier.astype(jnp.bfloat16),
        one_hot.astype(jnp.bfloat16),
        preferred_element_type=jnp.float32,
    )
    rank_in = jnp.sum(jnp.where(one_hot, before, 0.0), axis=1).astype(jnp.int32)
    target = (flat_routes * capacity + rank_in).reshape(top_count, out_rows)
    slots = expert_total * capacity
    middle, outbound = pl.pallas_call(
        middle_kernel,
        out_shape=(
            jax.ShapeDtypeStruct((out_rows, model_width), jnp.bfloat16),
            jax.ShapeDtypeStruct((slots, model_width), jnp.bfloat16),
        ),
        in_specs=[VMEM] * 7,
        out_specs=(VMEM, VMEM),
        compiler_params=pltpu.CompilerParams(vmem_limit_bytes=48 * 1024 * 1024),
    )(
        whole_rows,
        out_gain[None, :],
        out_proj,
        residual,
        mid_gain[None, :],
        mid_bias[None, :],
        target,
    )
    arrived = exchange_all(
        outbound.reshape(device_total, local_experts * capacity, model_width), sp_size, tp_size, 2
    )
    grouped_rows = arrived.reshape(device_total, local_experts, capacity, model_width)
    gate_part = jnp.einsum(
        "sekd,edf->sekf", grouped_rows, expert_gate, preferred_element_type=jnp.float32
    )
    up_part = jnp.einsum(
        "sekd,edf->sekf", grouped_rows, expert_up, preferred_element_type=jnp.float32
    )
    hidden = (jax.nn.silu(gate_part) * up_part).astype(jnp.bfloat16)
    served = jnp.einsum("sekf,efd->sekd", hidden, expert_down, preferred_element_type=jnp.float32)
    returned = exchange_all(
        served.astype(jnp.bfloat16).reshape(arrived.shape), sp_size, tp_size, 3
    )
    return pl.pallas_call(
        final_kernel,
        out_shape=jax.ShapeDtypeStruct((out_rows, model_width), jnp.bfloat16),
        in_specs=[VMEM] * 6,
        out_specs=VMEM,
        compiler_params=pltpu.CompilerParams(vmem_limit_bytes=48 * 1024 * 1024),
    )(
        returned.reshape(slots, model_width),
        target.T,
        route_weights,
        middle,
        final_gain[None, :],
        final_bias[None, :],
    )


def solution(mesh):
    return jax.shard_map(
        per_device,
        mesh=mesh,
        in_specs=(
            P("sp", "tp"),
            P("sp", "tp"),
            P("sp", "tp"),
            P("sp"),
            P(),
            P(),
            P(),
            P(),
            P(("sp", "tp"), None),
            P(),
            P(),
            P(("sp", "tp"), None),
            P(("sp", "tp"), None),
            P(("sp", "tp"), None, None),
            P(("sp", "tp"), None, None),
            P(("sp", "tp"), None, None),
            P(),
            P(),
        ),
        out_specs=P(("sp", "tp"), None),
        check_vma=False,
    )
```

```python
import functools

import jax
import jax.numpy as jnp
from jax import lax
from jax.experimental import pallas as pl
from jax.experimental.pallas import tpu as pltpu
from jax.sharding import PartitionSpec as P

HEAD = 128
GRID = 64


eps_norm = 1e-06
alpha_mix = 8.0**0.25
theta_base = 10000.0
score_factor = HEAD ** (-0.5) * 1.4426950408889634
VMEM = pl.BlockSpec(memory_space=pltpu.VMEM)
ANY = pl.BlockSpec(memory_space=pl.ANY)
SMEM = pl.BlockSpec(memory_space=pltpu.SMEM)


def rotary_tables(row_total, offset):
    positions = offset + jnp.arange(row_total, dtype=jnp.int32)
    grid_row = (positions // GRID).astype(jnp.float32)
    grid_col = (positions % GRID).astype(jnp.float32)
    pair_count = HEAD // 4
    inv_freq = theta_base ** (-jnp.arange(pair_count, dtype=jnp.float32) / pair_count)
    angles = jnp.concatenate(
        [grid_row[:, None] * inv_freq[None, :], grid_col[:, None] * inv_freq[None, :]], axis=1
    )
    return (jnp.cos(angles), jnp.sin(angles))


def normed_rotated(heads_in, gain_vec, cosine_table, sine_table):
    values = heads_in.astype(jnp.float32)
    inv_rms = lax.rsqrt(jnp.mean(values * values, axis=-1, keepdims=True) + eps_norm)
    values = values * inv_rms * gain_vec
    half_dim = HEAD // 2
    first_half = values[..., :half_dim]
    second_half = values[..., half_dim:]
    cosine_part = cosine_table[:, None, :]
    sine_part = sine_table[:, None, :]
    turned = jnp.concatenate(
        [
            first_half * cosine_part - second_half * sine_part,
            second_half * cosine_part + first_half * sine_part,
        ],
        axis=-1,
    )
    return turned.astype(jnp.bfloat16)


def layer_norm(stream, gain_vec, bias_vec):
    center = jnp.mean(stream, axis=-1, keepdims=True)
    spread = jnp.mean(jnp.square(stream - center), axis=-1, keepdims=True)
    return (stream - center) * lax.rsqrt(spread + eps_norm) * gain_vec + bias_vec


def barrier_with(peers):
    barrier = pltpu.get_barrier_semaphore()
    for peer in peers:
        pl.semaphore_signal(barrier, inc=1, device_id=peer, device_id_type=pl.DeviceIdType.MESH)
    pl.semaphore_wait(barrier, len(peers))


def gather_kernel(
    size, pair, kv_ref, doc_ref, kv_all, doc_all, kv_send, kv_recv, doc_send, doc_recv, own_sem
):
    me = lax.axis_index("sp")
    inner = lax.rem(me, pair)
    outer = me // pair
    outer_size = size // pair
    own = [
        pltpu.make_async_copy(kv_ref, kv_all.at[me], own_sem.at[0]),
        pltpu.make_async_copy(doc_ref, doc_all.at[me], own_sem.at[1]),
    ]
    for copy in own:
        copy.start()
    far = [
        lax.rem(outer + step, outer_size) * pair + inner for step in range(1, outer_size)
    ]
    mate = outer * pair + lax.rem(inner + 1, pair)
    peers = [{"sp": index} for index in far]
    if pair == 2:
        peers.append({"sp": mate})
    barrier_with(peers)

    def send(from_kv, from_doc, place, slot, target):
        copies = (
            pltpu.make_async_remote_copy(
                src_ref=from_kv,
                dst_ref=kv_all.at[place],
                send_sem=kv_send.at[slot],
                recv_sem=kv_recv.at[slot],
                device_id={"sp": target},
                device_id_type=pl.DeviceIdType.MESH,
            ),
            pltpu.make_async_remote_copy(
                src_ref=from_doc,
                dst_ref=doc_all.at[place],
                send_sem=doc_send.at[slot],
                recv_sem=doc_recv.at[slot],
                device_id={"sp": target},
                device_id_type=pl.DeviceIdType.MESH,
            ),
        )
        for copy in copies:
            copy.start()
        return copies

    far_copies = []
    for step, target in enumerate(far):
        far_copies.append(send(kv_ref, doc_ref, me, step, target))
    mate_copies = []
    if pair == 2:
        mate_copies.append(send(kv_ref, doc_ref, me, outer_size - 1, mate))
    for step in range(1, outer_size):
        for copy in far_copies[step - 1]:
            copy.wait_recv()
        if pair == 2:
            place = lax.rem(outer - step + outer_size, outer_size) * pair + inner
            mate_copies.append(
                send(kv_all.at[place], doc_all.at[place], place, outer_size - 1 + step, mate)
            )
    for copies in mate_copies:
        for copy in copies:
            copy.wait_recv()
    for copies in far_copies + mate_copies:
        for copy in copies:
            copy.wait_send()
    for copy in own:
        copy.wait()


def gather_keys(kv, docs, size):
    pair = 2 if size % 2 == 0 else 1
    slots = max(size - 1, 1)
    return pl.pallas_call(
        functools.partial(gather_kernel, size, pair),
        out_shape=(
            jax.ShapeDtypeStruct((size,) + kv.shape, kv.dtype),
            jax.ShapeDtypeStruct((size,) + docs.shape, docs.dtype),
        ),
        in_specs=[ANY, ANY],
        out_specs=(ANY, ANY),
        scratch_shapes=[pltpu.SemaphoreType.DMA((slots,)) for unused in range(4)]
        + [pltpu.SemaphoreType.DMA((2,))],
        compiler_params=pltpu.CompilerParams(collective_id=0, has_side_effects=True),
    )(kv, docs)


def attention_kernel(grouped, q_ref, qdoc_ref, kv_ref, doc_ref, range_ref, o_ref, m_ref, l_ref, acc_ref):
    rows = q_ref.shape[1]
    block = kv_ref.shape[2]
    pieces = doc_ref.shape[1]
    chunk = 256
    m_ref[...] = jnp.full(m_ref.shape, -1e30, jnp.float32)
    l_ref[...] = jnp.zeros(l_ref.shape, jnp.float32)
    acc_ref[...] = jnp.zeros(acc_ref.shape, jnp.float32)

    def advance(number, unused):
        keys = kv_ref[number, 0]
        values = kv_ref[number, 1]
        doc_rows = doc_ref[number]
        key_docs = jnp.concatenate([doc_rows[i : i + 1] for i in range(pieces)], axis=1)
        for head in range(grouped):
            for first in range(0, rows, chunk):
                part = pl.ds(first, chunk)
                scores = lax.dot_general(
                    q_ref[head, part],
                    keys,
                    (((1,), (1,)), ((), ())),
                    preferred_element_type=jnp.float32,
                )
                allowed = qdoc_ref[part, 0:1] == key_docs
                scores = jnp.where(allowed, scores * score_factor, -1e30)
                old_max = m_ref[head, part]
                new_max = jnp.maximum(old_max, jnp.max(scores, axis=1, keepdims=True))
                base = jnp.maximum(new_max[:, 0:1], -1e29)
                weights = jnp.exp2(scores - base)
                rescale = jnp.exp2(old_max - new_max)
                l_ref[head, part] = l_ref[head, part] * rescale + jnp.sum(
                    weights, axis=1, keepdims=True
                )
                acc_ref[head, part] = acc_ref[head, part] * rescale + jnp.dot(
                    weights.astype(jnp.bfloat16), values, preferred_element_type=jnp.float32
                )
                m_ref[head, part] = new_max
        return unused

    lax.fori_loop(range_ref[0], range_ref[1], advance, 0)
    for head in range(grouped):
        o_ref[:, head * HEAD : (head + 1) * HEAD] = (acc_ref[head] / l_ref[head]).astype(
            o_ref.dtype
        )


def attend(query_rot, query_docs, kv_all, doc_all, block_range):
    grouped, rows, width = query_rot.shape
    return pl.pallas_call(
        functools.partial(attention_kernel, grouped),
        out_shape=jax.ShapeDtypeStruct((rows, grouped * width), jnp.bfloat16),
        in_specs=[VMEM, VMEM, VMEM, VMEM, SMEM],
        out_specs=VMEM,
        scratch_shapes=[pltpu.VMEM((grouped, rows, width), jnp.float32) for unused in range(3)],
        compiler_params=pltpu.CompilerParams(vmem_limit_bytes=48 * 1024 * 1024),
    )(query_rot, query_docs, kv_all, doc_all, block_range)


def head_exchange_kernel(size, x_ref, o_ref, send_sem, recv_sem, own_sem):
    me = lax.axis_index("tp")
    rows, width = o_ref.shape[0], x_ref.shape[1]
    mine = o_ref.at[:, pl.ds(pl.multiple_of(me * width, width), width)]
    own = pltpu.make_async_copy(
        x_ref.at[pl.ds(pl.multiple_of(me * rows, rows), rows)], mine, own_sem
    )
    own.start()
    targets = [lax.rem(me + step, size) for step in range(1, size)]
    barrier_with([{"tp": target} for target in targets])
    copies = []
    for step, target in enumerate(targets):
        copy = pltpu.make_async_remote_copy(
            src_ref=x_ref.at[pl.ds(pl.multiple_of(target * rows, rows), rows)],
            dst_ref=mine,
            send_sem=send_sem.at[step],
            recv_sem=recv_sem.at[step],
            device_id={"tp": target},
            device_id_type=pl.DeviceIdType.MESH,
        )
        copy.start()
        copies.append(copy)
    for copy in copies:
        copy.wait()
    own.wait()


def exchange_heads(attention, size):
    rows, width = attention.shape
    return pl.pallas_call(
        functools.partial(head_exchange_kernel, size),
        out_shape=jax.ShapeDtypeStruct((rows // size, width * size), attention.dtype),
        in_specs=[VMEM],
        out_specs=VMEM,
        scratch_shapes=[
            pltpu.SemaphoreType.DMA((size,)),
            pltpu.SemaphoreType.DMA((size,)),
            pltpu.SemaphoreType.DMA,
        ],
        compiler_params=pltpu.CompilerParams(collective_id=1, has_side_effects=True),
    )(attention)


def flipped(number, pattern):
    bit = 1
    while bit <= pattern:
        if pattern & bit:
            number = number + bit - 2 * bit * lax.rem(number // bit, 2)
        bit *= 2
    return number


def expert_kernel(
    outer_size,
    inner_size,
    tp_size,
    x_ref,
    gate_ref,
    up_ref,
    down_ref,
    o_ref,
    held,
    served,
    out_send,
    out_recv,
    back_send,
    back_recv,
    own_sem,
):
    me = lax.axis_index("sp") * tp_size + lax.axis_index("tp")
    outer = me // inner_size
    inner = lax.rem(me, inner_size)
    size = outer_size * inner_size
    paired = outer_size & (outer_size - 1) == 0
    half = outer_size // 2
    upper, lower = list(range(half, outer_size)), list(range(1, half))
    if outer_size == 1:
        send_order, work_order = [0], [0]
    else:
        send_order = [group for group in upper + lower if group] + [0]
        work_order = [0] + [group for group in upper[:1] + lower + upper[1:] if group]

    def mesh_place(index):
        return {"sp": index // tp_size, "tp": lax.rem(index, tp_size)}

    def plane_to(group):
        if paired:
            return flipped(outer, group)
        return lax.rem(outer + group, outer_size)

    def plane_from(group):
        if paired:
            return flipped(outer, group)
        return lax.rem(outer - group + outer_size, outer_size)

    def target_of(group, step):
        return plane_to(group) * inner_size + lax.rem(inner + step, inner_size)

    def source_of(group, step):
        return plane_from(group) * inner_size + lax.rem(inner - step + inner_size, inner_size)

    def out_copy(group, step):
        target = target_of(group, step)
        return pltpu.make_async_remote_copy(
            src_ref=x_ref.at[target],
            dst_ref=held.at[me],
            send_sem=out_send.at[group * inner_size + step],
            recv_sem=out_recv.at[group * inner_size + step],
            device_id=mesh_place(target),
            device_id_type=pl.DeviceIdType.MESH,
        )

    def back_copy(group, step):
        source = source_of(group, step)
        return pltpu.make_async_remote_copy(
            src_ref=served.at[source],
            dst_ref=o_ref.at[me],
            send_sem=back_send.at[group * inner_size + step],
            recv_sem=back_recv.at[group * inner_size + step],
            device_id=mesh_place(source),
            device_id_type=pl.DeviceIdType.MESH,
        )

    def each(group, act):
        def once(step, unused):
            act(group, step)
            return unused

        lax.fori_loop(1 if group == 0 else 0, inner_size, once, 0)

    own_out = pltpu.make_async_copy(x_ref.at[me], held.at[me], own_sem.at[0])
    own_out.start()
    barrier = pltpu.get_barrier_semaphore()

    def greet(group, step):
        pl.semaphore_signal(
            barrier,
            inc=1,
            device_id=mesh_place(target_of(group, step)),
            device_id_type=pl.DeviceIdType.MESH,
        )

    for group in send_order:
        each(group, greet)
    pl.semaphore_wait(barrier, size - 1)
    for group in send_order:
        each(group, lambda g, step: out_copy(g, step).start())
    own_out.wait()
    local_experts = gate_ref.shape[0]
    block = held.shape[1]
    capacity = block // local_experts
    width = held.shape[2]
    for group in work_order:
        each(group, lambda g, step: out_copy(g, step).wait_recv())
        span = pl.ds(plane_from(group) * inner_size, inner_size)
        arrived = held[span]
        for expert in range(local_experts):
            part = slice(expert * capacity, (expert + 1) * capacity)
            rows = arrived[:, part].reshape(inner_size * capacity, width)
            gate = jnp.dot(rows, gate_ref[expert], preferred_element_type=jnp.float32)
            up = jnp.dot(rows, up_ref[expert], preferred_element_type=jnp.float32)
            hidden = (gate / (1.0 + jnp.exp(-gate)) * up).astype(jnp.bfloat16)
            result = jnp.dot(hidden, down_ref[expert], preferred_element_type=jnp.float32)
            served[span, part] = result.astype(jnp.bfloat16).reshape(inner_size, capacity, width)
        each(group, lambda g, step: back_copy(g, step).start())
    own_back = pltpu.make_async_copy(served.at[me], o_ref.at[me], own_sem.at[1])
    own_back.start()
    for group in work_order:
        each(group, lambda g, step: back_copy(g, step).wait_recv())
    for group in work_order:
        each(group, lambda g, step: out_copy(g, step).wait_send())
        each(group, lambda g, step: back_copy(g, step).wait_send())
    own_back.wait()


def run_experts(blocks, gate, up, down, sp_size, tp_size):
    size = blocks.shape[0]
    pair = 2 if sp_size % 2 == 0 else 1
    return pl.pallas_call(
        functools.partial(expert_kernel, sp_size // pair, pair * tp_size, tp_size),
        out_shape=jax.ShapeDtypeStruct(blocks.shape, blocks.dtype),
        in_specs=[VMEM] * 4,
        out_specs=VMEM,
        scratch_shapes=[pltpu.VMEM(blocks.shape, blocks.dtype) for unused in range(2)]
        + [pltpu.SemaphoreType.DMA((size,)) for unused in range(4)]
        + [pltpu.SemaphoreType.DMA((2,))],
        compiler_params=pltpu.CompilerParams(
            collective_id=2, has_side_effects=True, vmem_limit_bytes=48 * 1024 * 1024
        ),
    )(blocks, gate, up, down)


def middle_kernel(
    x_ref, gain_ref, proj_ref, res_ref, mid_gain_ref, mid_bias_ref, target_ref, mid_ref, out_ref
):
    whole = x_ref[...].astype(jnp.float32)
    mean_square = jnp.mean(whole * whole, axis=1, keepdims=True)
    scaled = (whole * gain_ref[...]).astype(jnp.bfloat16)
    projected = jnp.dot(scaled, proj_ref[...], preferred_element_type=jnp.float32)
    projected = projected * lax.rsqrt(mean_square + eps_norm)
    stream = alpha_mix * res_ref[...].astype(jnp.float32) + projected
    middle = layer_norm(stream, mid_gain_ref[...], mid_bias_ref[...]).astype(jnp.bfloat16)
    mid_ref[...] = middle
    slots, rows = out_ref.shape[0], middle.shape[0]
    slot = lax.broadcasted_iota(jnp.int32, (slots, rows), 0)
    chosen = slot == target_ref[0:1, :]
    for route in range(1, target_ref.shape[0]):
        chosen = chosen | (slot == target_ref[route : route + 1, :])
    select = jnp.where(chosen, 1.0, 0.0).astype(jnp.bfloat16)
    out_ref[...] = jnp.dot(select, middle, preferred_element_type=jnp.float32).astype(
        jnp.bfloat16
    )


def final_kernel(back_ref, target_ref, weight_ref, mid_ref, gain_ref, bias_ref, o_ref):
    rows, slots = mid_ref.shape[0], back_ref.shape[0]
    slot = lax.broadcasted_iota(jnp.int32, (rows, slots), 1)
    routed = None
    for route in range(target_ref.shape[1]):
        select = jnp.where(slot == target_ref[:, route : route + 1], 1.0, 0.0)
        picked = jnp.dot(
            select.astype(jnp.bfloat16), back_ref[...], preferred_element_type=jnp.float32
        )
        term = picked * weight_ref[:, route : route + 1]
        routed = term if routed is None else routed + term
    stream = alpha_mix * mid_ref[...].astype(jnp.float32) + routed
    o_ref[...] = layer_norm(stream, gain_ref[...], bias_ref[...]).astype(o_ref.dtype)


def per_device(
    queries,
    key_heads,
    value_heads,
    documents,
    query_gain,
    key_gain,
    out_gain,
    out_proj,
    residual,
    mid_gain,
    mid_bias,
    routes,
    route_weights,
    expert_gate,
    expert_up,
    expert_down,
    final_gain,
    final_bias,
):
    tok_rows = queries.shape[0]
    query_local = queries.shape[1] // HEAD
    key_local = key_heads.shape[1] // HEAD
    grouped = query_local // key_local
    sp_size = lax.axis_size("sp")
    tp_size = lax.axis_size("tp")
    offset = lax.axis_index("sp") * tok_rows
    cosine_table, sine_table = rotary_tables(tok_rows, offset)
    query_rot = normed_rotated(
        queries.reshape(tok_rows, query_local, HEAD), query_gain, cosine_table, sine_table
    )
    query_rot = jnp.transpose(query_rot, (1, 0, 2))
    key_rot = normed_rotated(
        key_heads.reshape(tok_rows, key_local, HEAD), key_gain, cosine_table, sine_table
    )
    values = value_heads.reshape(tok_rows, key_local, HEAD)
    query_docs = jnp.broadcast_to(documents[:, None], (tok_rows, HEAD))
    kv = jnp.transpose(jnp.stack([key_rot, values]), (2, 0, 1, 3))
    kv_all, doc_all = gather_keys(
        kv.reshape(key_local * 2, tok_rows, HEAD), documents.reshape(tok_rows // HEAD, HEAD), sp_size
    )
    low = jnp.sum((doc_all[:, -1, -1] < documents[0]).astype(jnp.int32))
    high = jnp.sum((doc_all[:, 0, 0] <= documents[tok_rows - 1]).astype(jnp.int32))
    block_range = jnp.stack([low, high])
    heads = []
    for head in range(key_local):
        heads.append(
            attend(
                query_rot[head * grouped : (head + 1) * grouped],
                query_docs,
                kv_all if key_local == 1 else kv_all[:, 2 * head : 2 * head + 2],
                doc_all,
                block_range,
            )
        )
    attention = heads[0] if key_local == 1 else jnp.concatenate(heads, axis=1)
    whole_rows = exchange_heads(attention, tp_size)
    out_rows, model_width = residual.shape
    top_count = routes.shape[1]
    local_experts = expert_gate.shape[0]
    device_total = sp_size * tp_size
    expert_total = local_experts * device_total
    capacity = 2 * out_rows * top_count // expert_total
    flat_routes = routes.T.reshape(-1)
    flat_total = flat_routes.shape[0]
    one_hot = flat_routes[:, None] == jnp.arange(expert_total, dtype=jnp.int32)[None, :]
    earlier = jnp.arange(flat_total)[:, None] > jnp.arange(flat_total)[None, :]
    before = jnp.dot(
        earlier.astype(jnp.bfloat16),
        one_hot.astype(jnp.bfloat16),
        preferred_element_type=jnp.float32,
    )
    rank_in = jnp.sum(jnp.where(one_hot, before, 0.0), axis=1).astype(jnp.int32)
    target = (flat_routes * capacity + rank_in).reshape(top_count, out_rows)
    slots = expert_total * capacity
    middle, outbound = pl.pallas_call(
        middle_kernel,
        out_shape=(
            jax.ShapeDtypeStruct((out_rows, model_width), jnp.bfloat16),
            jax.ShapeDtypeStruct((slots, model_width), jnp.bfloat16),
        ),
        in_specs=[VMEM] * 7,
        out_specs=(VMEM, VMEM),
        compiler_params=pltpu.CompilerParams(vmem_limit_bytes=48 * 1024 * 1024),
    )(
        whole_rows,
        out_gain[None, :],
        out_proj,
        residual,
        mid_gain[None, :],
        mid_bias[None, :],
        target,
    )
    returned = run_experts(
        outbound.reshape(device_total, local_experts * capacity, model_width),
        expert_gate,
        expert_up,
        expert_down,
        sp_size,
        tp_size,
    )
    return pl.pallas_call(
        final_kernel,
        out_shape=jax.ShapeDtypeStruct((out_rows, model_width), jnp.bfloat16),
        in_specs=[VMEM] * 6,
        out_specs=VMEM,
        compiler_params=pltpu.CompilerParams(vmem_limit_bytes=48 * 1024 * 1024),
    )(
        returned.reshape(slots, model_width),
        target.T,
        route_weights,
        middle,
        final_gain[None, :],
        final_bias[None, :],
    )


def solution(mesh):
    return jax.shard_map(
        per_device,
        mesh=mesh,
        in_specs=(
            P("sp", "tp"),
            P("sp", "tp"),
            P("sp", "tp"),
            P("sp"),
            P(),
            P(),
            P(),
            P(),
            P(("sp", "tp"), None),
            P(),
            P(),
            P(("sp", "tp"), None),
            P(("sp", "tp"), None),
            P(("sp", "tp"), None, None),
            P(("sp", "tp"), None, None),
            P(("sp", "tp"), None, None),
            P(),
            P(),
        ),
        out_specs=P(("sp", "tp"), None),
        check_vma=False,
    )
```

```python
import functools

import jax
import jax.numpy as jnp
from jax import lax
from jax.experimental import pallas as pl
from jax.experimental.pallas import tpu as pltpu
from jax.sharding import PartitionSpec as P

HEAD = 128
GRID = 64


eps_norm = 1e-06
alpha_mix = 8.0**0.25
theta_base = 10000.0
score_factor = HEAD ** (-0.5) * 1.4426950408889634
VMEM = pl.BlockSpec(memory_space=pltpu.VMEM)
ANY = pl.BlockSpec(memory_space=pl.ANY)
SMEM = pl.BlockSpec(memory_space=pltpu.SMEM)


def rotary_tables(row_total, offset):
    positions = offset + jnp.arange(row_total, dtype=jnp.int32)
    grid_row = (positions // GRID).astype(jnp.float32)
    grid_col = (positions % GRID).astype(jnp.float32)
    pair_count = HEAD // 4
    inv_freq = theta_base ** (-jnp.arange(pair_count, dtype=jnp.float32) / pair_count)
    angles = jnp.concatenate(
        [grid_row[:, None] * inv_freq[None, :], grid_col[:, None] * inv_freq[None, :]], axis=1
    )
    return (jnp.cos(angles), jnp.sin(angles))


def normed_rotated(heads_in, gain_vec, cosine_table, sine_table):
    values = heads_in.astype(jnp.float32)
    inv_rms = lax.rsqrt(jnp.mean(values * values, axis=-1, keepdims=True) + eps_norm)
    values = values * inv_rms * gain_vec
    half_dim = HEAD // 2
    first_half = values[..., :half_dim]
    second_half = values[..., half_dim:]
    cosine_part = cosine_table[:, None, :]
    sine_part = sine_table[:, None, :]
    turned = jnp.concatenate(
        [
            first_half * cosine_part - second_half * sine_part,
            second_half * cosine_part + first_half * sine_part,
        ],
        axis=-1,
    )
    return turned.astype(jnp.bfloat16)


def layer_norm(stream, gain_vec, bias_vec):
    center = jnp.mean(stream, axis=-1, keepdims=True)
    spread = jnp.mean(jnp.square(stream - center), axis=-1, keepdims=True)
    return (stream - center) * lax.rsqrt(spread + eps_norm) * gain_vec + bias_vec


def barrier_with(peers):
    barrier = pltpu.get_barrier_semaphore()
    for peer in peers:
        pl.semaphore_signal(barrier, inc=1, device_id=peer, device_id_type=pl.DeviceIdType.MESH)
    pl.semaphore_wait(barrier, len(peers))


def flipped(number, pattern):
    bit = 1
    while bit <= pattern:
        if pattern & bit:
            number = number + bit - 2 * bit * lax.rem(number // bit, 2)
        bit *= 2
    return number


def gather_kernel(
    size,
    pair,
    capacity,
    kv_ref,
    doc_ref,
    q_ref,
    q_gain_ref,
    cos_ref,
    sin_ref,
    route_ref,
    kv_all,
    doc_all,
    q_out,
    column_out,
    row_out,
    kv_send,
    kv_recv,
    doc_send,
    doc_recv,
    own_sem,
):
    me = lax.axis_index("sp")
    inner = lax.rem(me, pair)
    outer = me // pair
    outer_size = size // pair
    parts = kv_ref.shape[0]
    paired = outer_size & (outer_size - 1) == 0
    half = outer_size // 2
    upper, lower = list(range(half, outer_size)), list(range(1, half))
    send_order = [group for group in upper + lower if group]
    work_order = [group for group in upper[:1] + lower + upper[1:] if group]
    own = [
        pltpu.make_async_copy(kv_ref, kv_all.at[me], own_sem.at[0]),
        pltpu.make_async_copy(doc_ref, doc_all.at[me], own_sem.at[1]),
    ]
    for copy in own:
        copy.start()

    def plane(group, sign):
        if paired:
            return flipped(outer, group)
        return lax.rem(outer + sign * group + outer_size, outer_size)

    mate = outer * pair + lax.rem(inner + 1, pair)
    peers = [{"sp": plane(group, 1) * pair + inner} for group in send_order]
    if pair == 2:
        peers.append({"sp": mate})
    barrier_with(peers)

    def send(from_kv, from_doc, place, slot, target):
        copies = [
            pltpu.make_async_remote_copy(
                src_ref=from_kv.at[part],
                dst_ref=kv_all.at[place, part],
                send_sem=kv_send.at[slot, part],
                recv_sem=kv_recv.at[slot, part],
                device_id={"sp": target},
                device_id_type=pl.DeviceIdType.MESH,
            )
            for part in range(parts)
        ]
        copies.append(
            pltpu.make_async_remote_copy(
                src_ref=from_doc,
                dst_ref=doc_all.at[place],
                send_sem=doc_send.at[slot],
                recv_sem=doc_recv.at[slot],
                device_id={"sp": target},
                device_id_type=pl.DeviceIdType.MESH,
            )
        )
        return copies

    sent = []
    far_copies = {}
    for group in send_order:
        copies = send(kv_ref, doc_ref, me, group - 1, plane(group, 1) * pair + inner)
        far_copies[group] = copies
        for copy in copies:
            copy.start()
        sent += copies
    mate_copies = []
    if pair == 2:
        mate_copies += send(kv_ref, doc_ref, me, outer_size - 1, mate)
        for copy in mate_copies:
            copy.start()

    rows, width = q_out.shape[1], q_out.shape[2]
    cosine = jnp.concatenate([cos_ref[...], cos_ref[...]], axis=1)
    sine = jnp.concatenate([-sin_ref[...], sin_ref[...]], axis=1)
    for head in range(q_out.shape[0]):
        values = q_ref[:, head * width : (head + 1) * width].astype(jnp.float32)
        inv_rms = lax.rsqrt(jnp.mean(values * values, axis=1, keepdims=True) + eps_norm)
        values = values * inv_rms * q_gain_ref[...]
        crossed = jnp.concatenate([values[:, width // 2 :], values[:, : width // 2]], axis=1)
        q_out[head] = (values * cosine + crossed * sine).astype(jnp.bfloat16)

    tokens, top = column_out.shape
    experts = 2 * tokens * top // capacity
    down = lax.broadcasted_iota(jnp.int32, (tokens, tokens), 0)
    across = lax.broadcasted_iota(jnp.int32, (tokens, tokens), 1)
    earlier = jnp.where(down > across, 1.0, 0.0).astype(jnp.bfloat16)
    names = lax.broadcasted_iota(jnp.int32, (tokens, experts), 1)
    passed = jnp.zeros((1, experts), jnp.float32)
    for route in range(top):
        named = route_ref[:, route : route + 1]
        one_hot = jnp.where(names == named, 1.0, 0.0)
        before = passed + jnp.dot(
            earlier, one_hot.astype(jnp.bfloat16), preferred_element_type=jnp.float32
        )
        rank = jnp.sum(before * one_hot, axis=1, keepdims=True)
        slot = named.astype(jnp.float32) * capacity + rank
        column_out[:, route : route + 1] = slot.astype(jnp.int32)
        row = jnp.sum(jnp.where(down == across, slot, 0.0), axis=0, keepdims=True)
        row_out[route : route + 1, :] = row.astype(jnp.int32)
        passed = passed + jnp.sum(one_hot, axis=0, keepdims=True)

    for group in work_order:
        place = plane(group, -1) * pair + inner
        forward = []
        if pair == 2:
            forward = send(kv_all.at[place], doc_all.at[place], place, outer_size - 1 + group, mate)
        for number, copy in enumerate(far_copies[group]):
            copy.wait_recv()
            if pair == 2:
                forward[number].start()
        mate_copies += forward
    for copy in mate_copies:
        copy.wait_recv()
    for copy in sent + mate_copies:
        copy.wait_send()
    for copy in own:
        copy.wait()


def gather_keys(kv, docs, queries, query_gain, cosine_table, sine_table, routes, size, capacity):
    pair = 2 if size % 2 == 0 else 1
    slots = max(size - 1, 1)
    rows, width = queries.shape
    return pl.pallas_call(
        functools.partial(gather_kernel, size, pair, capacity),
        out_shape=(
            jax.ShapeDtypeStruct((size,) + kv.shape, kv.dtype),
            jax.ShapeDtypeStruct((size,) + docs.shape, docs.dtype),
            jax.ShapeDtypeStruct((width // HEAD, rows, HEAD), jnp.bfloat16),
            jax.ShapeDtypeStruct(routes.shape, jnp.int32),
            jax.ShapeDtypeStruct(routes.shape[::-1], jnp.int32),
        ),
        in_specs=[ANY, ANY] + [VMEM] * 5,
        out_specs=(ANY, ANY, VMEM, VMEM, VMEM),
        scratch_shapes=[
            pltpu.SemaphoreType.DMA((slots, kv.shape[0])),
            pltpu.SemaphoreType.DMA((slots, kv.shape[0])),
            pltpu.SemaphoreType.DMA((slots,)),
            pltpu.SemaphoreType.DMA((slots,)),
            pltpu.SemaphoreType.DMA((2,)),
        ],
        compiler_params=pltpu.CompilerParams(collective_id=0, has_side_effects=True),
    )(kv, docs, queries, query_gain[None, :], cosine_table, sine_table, routes)


def attention_kernel(grouped, q_ref, qdoc_ref, kv_ref, doc_ref, scalar_ref, o_ref, m_ref, l_ref, acc_ref):
    rows = q_ref.shape[1]
    block = kv_ref.shape[2]
    pieces = doc_ref.shape[1]
    chunk = 256
    m_ref[...] = jnp.full(m_ref.shape, -1e30, jnp.float32)
    l_ref[...] = jnp.zeros(l_ref.shape, jnp.float32)
    acc_ref[...] = jnp.zeros(acc_ref.shape, jnp.float32)

    def advance(number, unused):
        keys = kv_ref[number, 0]
        values = kv_ref[number, 1]
        doc_rows = doc_ref[number]
        key_docs = jnp.concatenate([doc_rows[i : i + 1] for i in range(pieces)], axis=1)
        for head in range(grouped):
            for first in range(0, rows, chunk):
                part = pl.ds(first, chunk)
                scores = lax.dot_general(
                    q_ref[head, part],
                    keys,
                    (((1,), (1,)), ((), ())),
                    preferred_element_type=jnp.float32,
                )
                allowed = qdoc_ref[part, 0:1] == key_docs
                scores = jnp.where(allowed, scores * score_factor, -1e30)
                old_max = m_ref[head, part]
                new_max = jnp.maximum(old_max, jnp.max(scores, axis=1, keepdims=True))
                base = jnp.maximum(new_max[:, 0:1], -1e29)
                weights = jnp.exp2(scores - base)
                rescale = jnp.exp2(old_max - new_max)
                l_ref[head, part] = l_ref[head, part] * rescale + jnp.sum(
                    weights, axis=1, keepdims=True
                )
                acc_ref[head, part] = acc_ref[head, part] * rescale + jnp.dot(
                    weights.astype(jnp.bfloat16), values, preferred_element_type=jnp.float32
                )
                m_ref[head, part] = new_max
        return unused

    mine = lax.axis_index("sp")
    first_doc = scalar_ref[mine, 0, 0]
    last_doc = scalar_ref[mine, pieces - 1, HEAD - 1]

    def count(number, bounds):
        low, high = bounds
        low = low + (scalar_ref[number, pieces - 1, HEAD - 1] < first_doc).astype(jnp.int32)
        high = high + (scalar_ref[number, 0, 0] <= last_doc).astype(jnp.int32)
        return low, high

    low, high = lax.fori_loop(0, doc_ref.shape[0], count, (jnp.int32(0), jnp.int32(0)))
    lax.fori_loop(low, high, advance, 0)
    for head in range(grouped):
        o_ref[:, head * HEAD : (head + 1) * HEAD] = (acc_ref[head] / l_ref[head]).astype(
            o_ref.dtype
        )


def attend(query_rot, query_docs, kv_all, doc_all):
    grouped, rows, width = query_rot.shape
    return pl.pallas_call(
        functools.partial(attention_kernel, grouped),
        out_shape=jax.ShapeDtypeStruct((rows, grouped * width), jnp.bfloat16),
        in_specs=[VMEM, VMEM, VMEM, VMEM, SMEM],
        out_specs=VMEM,
        scratch_shapes=[pltpu.VMEM((grouped, rows, width), jnp.float32) for unused in range(3)],
        compiler_params=pltpu.CompilerParams(vmem_limit_bytes=48 * 1024 * 1024),
    )(query_rot, query_docs, kv_all, doc_all, doc_all)


def head_exchange_kernel(size, x_ref, o_ref, send_sem, recv_sem, own_sem):
    me = lax.axis_index("tp")
    rows, width = o_ref.shape[0], x_ref.shape[1]
    mine = o_ref.at[:, pl.ds(pl.multiple_of(me * width, width), width)]
    own = pltpu.make_async_copy(
        x_ref.at[pl.ds(pl.multiple_of(me * rows, rows), rows)], mine, own_sem
    )
    own.start()
    targets = [lax.rem(me + step, size) for step in range(1, size)]
    barrier_with([{"tp": target} for target in targets])
    copies = []
    for step, target in enumerate(targets):
        copy = pltpu.make_async_remote_copy(
            src_ref=x_ref.at[pl.ds(pl.multiple_of(target * rows, rows), rows)],
            dst_ref=mine,
            send_sem=send_sem.at[step],
            recv_sem=recv_sem.at[step],
            device_id={"tp": target},
            device_id_type=pl.DeviceIdType.MESH,
        )
        copy.start()
        copies.append(copy)
    for copy in copies:
        copy.wait()
    own.wait()


def exchange_heads(attention, size):
    rows, width = attention.shape
    return pl.pallas_call(
        functools.partial(head_exchange_kernel, size),
        out_shape=jax.ShapeDtypeStruct((rows // size, width * size), attention.dtype),
        in_specs=[VMEM],
        out_specs=VMEM,
        scratch_shapes=[
            pltpu.SemaphoreType.DMA((size,)),
            pltpu.SemaphoreType.DMA((size,)),
            pltpu.SemaphoreType.DMA,
        ],
        compiler_params=pltpu.CompilerParams(collective_id=1, has_side_effects=True),
    )(attention)


def expert_kernel(
    outer_size,
    inner_size,
    tp_size,
    x_ref,
    gate_ref,
    up_ref,
    down_ref,
    o_ref,
    held,
    served,
    out_send,
    out_recv,
    back_send,
    back_recv,
    own_sem,
):
    me = lax.axis_index("sp") * tp_size + lax.axis_index("tp")
    outer = me // inner_size
    inner = lax.rem(me, inner_size)
    size = outer_size * inner_size
    paired = outer_size & (outer_size - 1) == 0
    half = outer_size // 2
    upper, lower = list(range(half, outer_size)), list(range(1, half))
    if outer_size == 1:
        send_order, work_order = [0], [0]
    else:
        send_order = [group for group in upper + lower if group] + [0]
        work_order = [0] + [group for group in upper[:1] + lower + upper[1:] if group]

    def mesh_place(index):
        return {"sp": index // tp_size, "tp": lax.rem(index, tp_size)}

    def plane_to(group):
        if paired:
            return flipped(outer, group)
        return lax.rem(outer + group, outer_size)

    def plane_from(group):
        if paired:
            return flipped(outer, group)
        return lax.rem(outer - group + outer_size, outer_size)

    def target_of(group, step):
        return plane_to(group) * inner_size + lax.rem(inner + step, inner_size)

    def source_of(group, step):
        return plane_from(group) * inner_size + lax.rem(inner - step + inner_size, inner_size)

    def out_copy(group, step):
        target = target_of(group, step)
        return pltpu.make_async_remote_copy(
            src_ref=x_ref.at[target],
            dst_ref=held.at[me],
            send_sem=out_send.at[group * inner_size + step],
            recv_sem=out_recv.at[group * inner_size + step],
            device_id=mesh_place(target),
            device_id_type=pl.DeviceIdType.MESH,
        )

    def back_copy(group, step):
        source = source_of(group, step)
        return pltpu.make_async_remote_copy(
            src_ref=served.at[source],
            dst_ref=o_ref.at[me],
            send_sem=back_send.at[group * inner_size + step],
            recv_sem=back_recv.at[group * inner_size + step],
            device_id=mesh_place(source),
            device_id_type=pl.DeviceIdType.MESH,
        )

    def each(group, act):
        def once(step, unused):
            act(group, step)
            return unused

        lax.fori_loop(1 if group == 0 else 0, inner_size, once, 0)

    own_out = pltpu.make_async_copy(x_ref.at[me], held.at[me], own_sem.at[0])
    own_out.start()
    barrier = pltpu.get_barrier_semaphore()

    def greet(group, step):
        pl.semaphore_signal(
            barrier,
            inc=1,
            device_id=mesh_place(target_of(group, step)),
            device_id_type=pl.DeviceIdType.MESH,
        )

    for group in send_order:
        each(group, greet)
    pl.semaphore_wait(barrier, size - 1)
    for group in send_order:
        each(group, lambda g, step: out_copy(g, step).start())
    own_out.wait()
    local_experts = gate_ref.shape[0]
    block = held.shape[1]
    capacity = block // local_experts
    width = held.shape[2]
    for group in work_order:
        each(group, lambda g, step: out_copy(g, step).wait_recv())
        span = pl.ds(plane_from(group) * inner_size, inner_size)
        arrived = held[span]
        for expert in range(local_experts):
            part = slice(expert * capacity, (expert + 1) * capacity)
            rows = arrived[:, part].reshape(inner_size * capacity, width)
            gate = jnp.dot(rows, gate_ref[expert], preferred_element_type=jnp.float32)
            up = jnp.dot(rows, up_ref[expert], preferred_element_type=jnp.float32)
            hidden = (gate / (1.0 + jnp.exp(-gate)) * up).astype(jnp.bfloat16)
            result = jnp.dot(hidden, down_ref[expert], preferred_element_type=jnp.float32)
            served[span, part] = result.astype(jnp.bfloat16).reshape(inner_size, capacity, width)
        each(group, lambda g, step: back_copy(g, step).start())
    own_back = pltpu.make_async_copy(served.at[me], o_ref.at[me], own_sem.at[1])
    own_back.start()
    for group in work_order:
        each(group, lambda g, step: back_copy(g, step).wait_recv())
    for group in work_order:
        each(group, lambda g, step: out_copy(g, step).wait_send())
        each(group, lambda g, step: back_copy(g, step).wait_send())
    own_back.wait()


def run_experts(blocks, gate, up, down, sp_size, tp_size):
    size = blocks.shape[0]
    pair = 2 if sp_size % 2 == 0 else 1
    return pl.pallas_call(
        functools.partial(expert_kernel, sp_size // pair, pair * tp_size, tp_size),
        out_shape=jax.ShapeDtypeStruct(blocks.shape, blocks.dtype),
        in_specs=[VMEM] * 4,
        out_specs=VMEM,
        scratch_shapes=[pltpu.VMEM(blocks.shape, blocks.dtype) for unused in range(2)]
        + [pltpu.SemaphoreType.DMA((size,)) for unused in range(4)]
        + [pltpu.SemaphoreType.DMA((2,))],
        compiler_params=pltpu.CompilerParams(
            collective_id=2, has_side_effects=True, vmem_limit_bytes=48 * 1024 * 1024
        ),
    )(blocks, gate, up, down)


def middle_kernel(
    x_ref, gain_ref, proj_ref, res_ref, mid_gain_ref, mid_bias_ref, target_ref, mid_ref, out_ref
):
    whole = x_ref[...].astype(jnp.float32)
    mean_square = jnp.mean(whole * whole, axis=1, keepdims=True)
    scaled = (whole * gain_ref[...]).astype(jnp.bfloat16)
    projected = jnp.dot(scaled, proj_ref[...], preferred_element_type=jnp.float32)
    projected = projected * lax.rsqrt(mean_square + eps_norm)
    stream = alpha_mix * res_ref[...].astype(jnp.float32) + projected
    middle = layer_norm(stream, mid_gain_ref[...], mid_bias_ref[...]).astype(jnp.bfloat16)
    mid_ref[...] = middle
    slots, rows = out_ref.shape[0], middle.shape[0]
    slot = lax.broadcasted_iota(jnp.int32, (slots, rows), 0)
    chosen = slot == target_ref[0:1, :]
    for route in range(1, target_ref.shape[0]):
        chosen = chosen | (slot == target_ref[route : route + 1, :])
    select = jnp.where(chosen, 1.0, 0.0).astype(jnp.bfloat16)
    out_ref[...] = jnp.dot(select, middle, preferred_element_type=jnp.float32).astype(
        jnp.bfloat16
    )


def final_kernel(back_ref, target_ref, weight_ref, mid_ref, gain_ref, bias_ref, o_ref):
    rows, slots = mid_ref.shape[0], back_ref.shape[0]
    slot = lax.broadcasted_iota(jnp.int32, (rows, slots), 1)
    routed = None
    for route in range(target_ref.shape[1]):
        select = jnp.where(slot == target_ref[:, route : route + 1], 1.0, 0.0)
        picked = jnp.dot(
            select.astype(jnp.bfloat16), back_ref[...], preferred_element_type=jnp.float32
        )
        term = picked * weight_ref[:, route : route + 1]
        routed = term if routed is None else routed + term
    stream = alpha_mix * mid_ref[...].astype(jnp.float32) + routed
    o_ref[...] = layer_norm(stream, gain_ref[...], bias_ref[...]).astype(o_ref.dtype)


def per_device(
    queries,
    key_heads,
    value_heads,
    documents,
    query_gain,
    key_gain,
    out_gain,
    out_proj,
    residual,
    mid_gain,
    mid_bias,
    routes,
    route_weights,
    expert_gate,
    expert_up,
    expert_down,
    final_gain,
    final_bias,
):
    tok_rows = queries.shape[0]
    query_local = queries.shape[1] // HEAD
    key_local = key_heads.shape[1] // HEAD
    grouped = query_local // key_local
    sp_size = lax.axis_size("sp")
    tp_size = lax.axis_size("tp")
    offset = lax.axis_index("sp") * tok_rows
    cosine_table, sine_table = rotary_tables(tok_rows, offset)
    key_rot = normed_rotated(
        key_heads.reshape(tok_rows, key_local, HEAD), key_gain, cosine_table, sine_table
    )
    values = value_heads.reshape(tok_rows, key_local, HEAD)
    query_docs = jnp.broadcast_to(documents[:, None], (tok_rows, HEAD))
    kv = jnp.transpose(jnp.stack([key_rot, values]), (2, 0, 1, 3))
    out_rows, model_width = residual.shape
    top_count = routes.shape[1]
    local_experts = expert_gate.shape[0]
    device_total = sp_size * tp_size
    expert_total = local_experts * device_total
    capacity = 2 * out_rows * top_count // expert_total
    kv_all, doc_all, query_rot, target_columns, target_rows = gather_keys(
        kv.reshape(key_local * 2, tok_rows, HEAD),
        documents.reshape(tok_rows // HEAD, HEAD),
        queries,
        query_gain,
        cosine_table,
        sine_table,
        routes,
        sp_size,
        capacity,
    )
    heads = []
    for head in range(key_local):
        heads.append(
            attend(
                query_rot[head * grouped : (head + 1) * grouped],
                query_docs,
                kv_all if key_local == 1 else kv_all[:, 2 * head : 2 * head + 2],
                doc_all,
            )
        )
    attention = heads[0] if key_local == 1 else jnp.concatenate(heads, axis=1)
    whole_rows = exchange_heads(attention, tp_size)
    slots = expert_total * capacity
    middle, outbound = pl.pallas_call(
        middle_kernel,
        out_shape=(
            jax.ShapeDtypeStruct((out_rows, model_width), jnp.bfloat16),
            jax.ShapeDtypeStruct((slots, model_width), jnp.bfloat16),
        ),
        in_specs=[VMEM] * 7,
        out_specs=(VMEM, VMEM),
        compiler_params=pltpu.CompilerParams(vmem_limit_bytes=48 * 1024 * 1024),
    )(
        whole_rows,
        out_gain[None, :],
        out_proj,
        residual,
        mid_gain[None, :],
        mid_bias[None, :],
        target_rows,
    )
    returned = run_experts(
        outbound.reshape(device_total, local_experts * capacity, model_width),
        expert_gate,
        expert_up,
        expert_down,
        sp_size,
        tp_size,
    )
    return pl.pallas_call(
        final_kernel,
        out_shape=jax.ShapeDtypeStruct((out_rows, model_width), jnp.bfloat16),
        in_specs=[VMEM] * 6,
        out_specs=VMEM,
        compiler_params=pltpu.CompilerParams(vmem_limit_bytes=48 * 1024 * 1024),
    )(
        returned.reshape(slots, model_width),
        target_columns,
        route_weights,
        middle,
        final_gain[None, :],
        final_bias[None, :],
    )


def solution(mesh):
    return jax.shard_map(
        per_device,
        mesh=mesh,
        in_specs=(
            P("sp", "tp"),
            P("sp", "tp"),
            P("sp", "tp"),
            P("sp"),
            P(),
            P(),
            P(),
            P(),
            P(("sp", "tp"), None),
            P(),
            P(),
            P(("sp", "tp"), None),
            P(("sp", "tp"), None),
            P(("sp", "tp"), None, None),
            P(("sp", "tp"), None, None),
            P(("sp", "tp"), None, None),
            P(),
            P(),
        ),
        out_specs=P(("sp", "tp"), None),
        check_vma=False,
    )
```
